32 devices in a mesh: grp: 2 (over y), fs: 4 (over z), tp: 4 (over x, core).
Axes of the slice: x: 2, y: 2, z: 4, core: 2. Of those that a mesh axis runs over, the one named last changes fastest.
Arguments:
- tokens: bfloat16 [4096, 2048], P(('grp', 'fs', 'tp')), parts along dimension 0, may hold values from -6 to 6
- mix_weight_in: bfloat16 [2048, 1024], P('fs', 'tp'), may hold values from -0.125 to 0.125
- pool_scale: float32 [1024], P('tp'), may hold values from 0.1 to 1.9
- mix_weight_out: bfloat16 [1024, 2048], P('tp', 'fs'), may hold values from -0.1875 to 0.1875
- up_weight: bfloat16 [2048, 8192], P('fs', 'tp'), may hold values from -0.125 to 0.125
- down_weight: bfloat16 [8192, 2048], P('tp', 'fs'), may hold values from -0.0625 to 0.0625
- gains: float32 [4, 2048], replicated, may hold values from 0.1 to 1.9
Outputs:
- result: bfloat16 [4096, 2048], P(('grp', 'fs', 'tp')), parts along dimension 0
The draws below stay inside these ranges and needn't reach their ends.
There are 2 independent parts, one for each index of `grp`. The reference program is written for one: setup_inputs(seed, part) draws one part's arguments, and reference() takes and returns one part's arrays. A program takes and returns all parts, laid end to end along the dimension named above; an argument that names none is the same for every part. Nothing has to cross between parts.
All inputs are finite; a program needn't handle non-finite values.
Results may differ from the reference program's by a relative error of at most 0.02.
Values may be sent and summed in bfloat16 or wider, within the bound.
No kernel may reach another device: no remote copies, remote signals or barrier semaphores. Data moves between devices by JAX's collectives and lax.ppermute only.
A program may use at most 64 MiB of HBM per device.

```python
import jax
import jax.numpy as jnp
from jax import lax

D = 2048
PW = 1024
GROUPS = 4
FF = 8192
ROWS = 128
TOKENS = 2048
N_FS = 4
N_TP = 4


def level_of(own_key, extent, split, least, top_value):
    factor_of, own = 1.0, jax.random.fold_in(own_key, 6)
    for dim, blocks in split:
        heights = jnp.exp(jax.random.uniform(jax.random.fold_in(own, dim), (blocks,), jnp.float32, least / len(split), top_value / len(split)))
        factor_of = factor_of * jnp.repeat(heights, extent[dim] // blocks).reshape([-1 if axis == dim else 1 for axis in range(len(extent))])
    return factor_of


def scatter_about(key, shape, spread, reach, shards=(), kind=jnp.bfloat16):
    level = level_of(key, shape, shards, -0.22, 0.18) if shards else 1.0
    entries = jax.random.normal(key, shape, jnp.float32) * spread * level
    return jnp.minimum(jnp.maximum(entries, -reach), reach).astype(kind)


def setup_inputs(seed: int = 0, part: int = 0) -> dict:
    keys = jax.random.split(jax.random.key(seed), 8)
    own_keys = jax.random.split(jax.random.fold_in(keys[7], part), 8)
    return {
        "tokens": scatter_about(own_keys[0], (TOKENS, D), 1.0, 6.0, ((0, 16),)),
        "mix_weight_in": scatter_about(keys[1], (D, PW), D ** -0.5, 0.125, ((0, 4), (1, 4))),
        "pool_scale": jnp.clip(1.0 + 0.18 * jax.random.normal(keys[2], (PW,), jnp.float32), 0.1, 1.9),
        "mix_weight_out": scatter_about(keys[3], (PW, D), PW ** -0.5, 0.1875, ((0, 4), (1, 4))),
        "up_weight": scatter_about(keys[4], (D, FF), D ** -0.5, 0.125, ((0, 4), (1, 4))),
        "down_weight": scatter_about(keys[5], (FF, D), FF ** -0.5, 0.0625, ((0, 4), (1, 4))),
        "gains": jnp.clip(1.0 + 0.18 * jax.random.normal(keys[6], (4, D), jnp.float32), 0.1, 1.9),
    }


norm_eps = 1e-06
pool_spans = (2, 4, 8, 16)

def normalize(values, gain):
    upcast = values.astype(jnp.float32)
    return upcast * lax.rsqrt(lax.optimization_barrier(jnp.mean(upcast * upcast, axis=-1, keepdims=True)) + norm_eps) * gain

def pooling(mixed_in):
    length = mixed_in.shape[0]
    upcast = mixed_in.astype(jnp.float32)
    running = jnp.cumsum(upcast, axis=0)
    position = jnp.arange(1, length + 1, dtype=jnp.float32)[:, None]
    group_of = (jnp.arange(PW) // (PW // GROUPS))[None, :]
    average = jnp.zeros_like(upcast)
    for index, span in enumerate(pool_spans):
        lagged = jnp.pad(running, ((span, 0), (0, 0)))[:length]
        window_mean = (running - lagged) / jnp.minimum(position, float(span))
        average = jnp.where(group_of == index, window_mean, average)
    return average - upcast

def split_sum(left, right, width):
    total = jnp.zeros((left.shape[0], right.shape[1]), jnp.float32)
    for block in range(N_TP):
        partial_value = jnp.dot(left[:, block * width:(block + 1) * width], right[block * width:(block + 1) * width], preferred_element_type=jnp.float32)
        total = total + lax.optimization_barrier(partial_value.astype(jnp.bfloat16)).astype(jnp.float32)
    return total.astype(jnp.bfloat16)

def reference(tokens, mix_weight_in, pool_scale, mix_weight_out, up_weight, down_weight, gains):

    def one_sequence(sequence):
        normed = normalize(sequence, gains[0]).astype(jnp.bfloat16)
        mixed_in = jnp.dot(normed, mix_weight_in, preferred_element_type=jnp.float32).astype(jnp.bfloat16)
        scaled = (pooling(mixed_in) * pool_scale).astype(jnp.bfloat16)
        mixer_out = split_sum(scaled, mix_weight_out, PW // N_TP)
        middle = (sequence.astype(jnp.float32) + normalize(mixer_out, gains[1])).astype(jnp.bfloat16)
        normed_two = normalize(middle, gains[2]).astype(jnp.bfloat16)
        hidden_pre = jax.nn.relu(jnp.dot(normed_two, up_weight, preferred_element_type=jnp.float32))
        squared = (hidden_pre * hidden_pre).astype(jnp.bfloat16)
        channel_out = split_sum(squared, down_weight, FF // N_TP)
        return (middle.astype(jnp.float32) + normalize(channel_out, gains[3])).astype(jnp.bfloat16)
    sequences = tokens.reshape(N_FS, ROWS * N_TP, D)
    return lax.map(one_sequence, sequences).reshape(TOKENS, D)
```

```python
import jax
import jax.numpy as jnp
from jax import lax
from jax.sharding import PartitionSpec as P

PW = 1024
GROUPS = 4

norm_eps = 1e-06
pool_spans = (2, 4, 8, 16)


f32, bf16 = jnp.float32, jnp.bfloat16


def normalize(values, gain):
    upcast = values.astype(jnp.float32)
    return upcast * lax.rsqrt(jnp.mean(upcast * upcast, axis=-1, keepdims=True) + norm_eps) * gain


def pooling(mixed_in, first_channel):
    length = mixed_in.shape[0]
    upcast = mixed_in.astype(jnp.float32)
    running = jnp.cumsum(upcast, axis=0)
    position = jnp.arange(1, length + 1, dtype=jnp.float32)[:, None]
    channel = first_channel + jnp.arange(mixed_in.shape[1], dtype=jnp.int32)
    group_of = (channel // (PW // GROUPS))[None, :]
    average = jnp.zeros_like(upcast)
    for index, span in enumerate(pool_spans):
        lagged = jnp.pad(running, ((span, 0), (0, 0)))[:length]
        window_mean = (running - lagged) / jnp.minimum(position, float(span))
        average = jnp.where(group_of == index, window_mean, average)
    return average - upcast


def whole_axis(tokens, mix_weight_in, pool_scale, mix_weight_out, up_weight, down_weight, gains):
    normed = normalize(tokens, gains[0]).astype(jnp.bfloat16)
    gathered = lax.all_gather(normed, "tp", axis=0, tiled=True)
    mixed_acc = jnp.dot(
        gathered,
        lax.all_gather(mix_weight_in, "fs", axis=0, tiled=True),
        preferred_element_type=jnp.float32,
    )
    weight_out = lax.all_gather(mix_weight_out, "fs", axis=1, tiled=True)
    mixed_in = mixed_acc.astype(jnp.bfloat16)
    first_channel = lax.axis_index("tp") * mix_weight_in.shape[1]
    scaled = (pooling(mixed_in, first_channel) * pool_scale).astype(jnp.bfloat16)
    picked = scaled
    mixer_out = lax.psum_scatter(
        jnp.dot(picked, weight_out, preferred_element_type=jnp.float32).astype(jnp.bfloat16),
        "tp",
        scatter_dimension=0,
        tiled=True,
    )
    middle = (tokens.astype(jnp.float32) + normalize(mixer_out, gains[1])).astype(jnp.bfloat16)
    normed_two = normalize(middle, gains[2]).astype(jnp.bfloat16)
    gathered_two = lax.all_gather(normed_two, "tp", axis=0, tiled=True)
    whole_up = lax.all_gather(up_weight, "fs", axis=0, tiled=True)
    hidden_pre = jnp.dot(gathered_two, whole_up, preferred_element_type=jnp.float32)
    hidden_pre = jax.nn.relu(hidden_pre)
    squared = (hidden_pre * hidden_pre).astype(jnp.bfloat16)
    whole_down = lax.all_gather(down_weight, "fs", axis=1, tiled=True)
    picked = squared
    channel_out = lax.psum_scatter(
        jnp.dot(picked, whole_down, preferred_element_type=jnp.float32).astype(jnp.bfloat16),
        "tp",
        scatter_dimension=0,
        tiled=True,
    )
    return (middle.astype(jnp.float32) + normalize(channel_out, gains[3])).astype(jnp.bfloat16)


def rsqrt_mean(blocks, width):
    total = sum(jnp.sum(b.astype(f32) * b.astype(f32), axis=-1, keepdims=True) for b in blocks)
    return lax.rsqrt(total / width + norm_eps)


def dot(a, b):
    return jnp.dot(a, b, preferred_element_type=f32)


def make_local(n_grp, n_fs, n_tp):
    def swap(value, axis, n, bit):
        return lax.ppermute(value, axis, [(i, i ^ bit) for i in range(n)])

    def local(tokens, mix_in, pool_scale, mix_out, up, down, gains):
        g, z, t = lax.axis_index("grp"), lax.axis_index("fs"), lax.axis_index("tp")
        rows, width = tokens.shape
        col = width // n_fs
        channels = mix_in.shape[1]
        part = channels // n_grp
        ff = up.shape[1] // n_grp

        def slots(value):
            blocks = [value[..., k * col:(k + 1) * col] for k in range(n_fs)]
            for bit in (2, 1):
                blocks = [jnp.where((z & bit) != 0, blocks[k ^ bit], blocks[k]) for k in range(n_fs)]
            return blocks

        def gather_fs(value):
            two = swap(value, "fs", n_fs, 2)
            one = swap(value, "fs", n_fs, 1)
            three = swap(two, "fs", n_fs, 1)
            return [value, one, two, three]

        mi = gather_fs(lax.dynamic_slice_in_dim(mix_in, g * part, part, axis=1))
        mo = gather_fs(lax.dynamic_slice_in_dim(mix_out, g * part, part, axis=0))
        up = gather_fs(lax.dynamic_slice_in_dim(up, g * ff, ff, axis=1))
        down = lax.dynamic_slice_in_dim(down, g * ff, ff, axis=0)
        down_a = gather_fs(down[:, :col // 2])
        down_b = gather_fs(down[:, col // 2:])

        w_in = jnp.concatenate(mi, axis=0)
        w_in = jnp.concatenate([w_in, swap(w_in, "grp", n_grp, 1)], axis=1)
        w_out = jnp.concatenate(mo, axis=1)
        w_out = jnp.concatenate([w_out, swap(w_out, "grp", n_grp, 1)], axis=0)

        gain = [slots(gains[k:k + 1]) for k in range(4)]
        x = slots(tokens)
        r = rsqrt_mean([tokens], width)
        normed = jnp.concatenate([(x[j].astype(f32) * r * gain[0][j]).astype(bf16) for j in range(n_fs)], axis=1)
        gathered = jnp.concatenate([normed, swap(normed, "tp", n_tp, 2)], axis=0)
        gathered = jnp.concatenate([gathered, swap(gathered, "tp", n_tp, 1)], axis=0)
        order = (0, 2, 1, 3)

        scale = [lax.dynamic_slice_in_dim(pool_scale, (g ^ k) * part, part) for k in range(n_grp)]
        scale = jnp.concatenate(scale)[None, :]
        index = jnp.arange(rows, dtype=jnp.int32)
        position = jnp.concatenate([(t ^ k) * rows + index for k in order])
        group = PW // GROUPS
        mine = (t * channels) // group
        span = jnp.int32(pool_spans[0])
        for k in range(1, GROUPS):
            span = jnp.where(mine == k, pool_spans[k], span)
        lag = position[:, None] - position[None, :]
        ones = ((lag >= 0) & (lag < span)).astype(bf16)
        count = jnp.minimum(position + 1, span).astype(f32)[:, None]

        mixed = dot(gathered, w_in).astype(bf16)
        average = dot(ones, mixed) / count
        scaled = ((average - mixed.astype(f32)) * scale).astype(bf16)
        half = 2 * rows
        sent = swap(dot(scaled[half:], w_out).astype(bf16), "tp", n_tp, 1)
        partial = (dot(scaled[:half], w_out) + sent.astype(f32)).astype(bf16)
        sent = swap(partial[rows:], "tp", n_tp, 2)
        partial = (partial[:rows].astype(f32) + sent.astype(f32)).astype(bf16)

        mixer_out = [partial[:, k * col:(k + 1) * col] for k in range(n_fs)]
        r = rsqrt_mean(mixer_out, width)
        middle = [(x[j].astype(f32) + mixer_out[j].astype(f32) * r * gain[1][j]).astype(bf16) for j in range(n_fs)]
        r = rsqrt_mean(middle, width)
        normed_two = [(middle[j].astype(f32) * r * gain[2][j]).astype(bf16) for j in range(n_fs)]

        left = jnp.concatenate(normed_two[:2], axis=1)
        right = jnp.concatenate(normed_two[2:], axis=1)
        left = jnp.concatenate([left, swap(left, "tp", n_tp, 2)], axis=0)
        left_far = swap(left, "grp", n_grp, 1)
        right_grp = swap(right, "grp", n_grp, 1)
        right_far = swap(jnp.concatenate([right, right_grp], axis=0), "tp", n_tp, 2)
        chips = jnp.concatenate(
            [
                jnp.concatenate([left, left_far], axis=0),
                jnp.concatenate([right, right_far[:rows], right_grp, right_far[rows:]], axis=0),
            ],
            axis=1,
        )
        everything = jnp.concatenate([chips, swap(chips, "tp", n_tp, 1)], axis=0)

        hidden = sum(dot(everything[:, j * col:(j + 1) * col], up[j]) for j in range(n_fs))
        hidden = jnp.maximum(hidden, 0.0)
        squared = (hidden * hidden).astype(bf16)

        def add_up(weights):
            half = 4 * rows
            sent = jnp.concatenate([dot(squared[half:], w).astype(bf16) for w in weights], axis=1)
            got = swap(sent, "tp", n_tp, 1)
            spans, at = [], 0
            for w in weights:
                spans.append((at, at + w.shape[1]))
                at += w.shape[1]
            total = [(dot(squared[:half], w) + got[:, a:b].astype(f32)).astype(bf16) for w, (a, b) in zip(weights, spans)]
            got = swap(jnp.concatenate([v[half // 2:] for v in total], axis=1), "grp", n_grp, 1)
            total = [(v[:half // 2].astype(f32) + got[:, a:b].astype(f32)).astype(bf16) for v, (a, b) in zip(total, spans)]
            got = swap(jnp.concatenate([v[rows:] for v in total], axis=1), "tp", n_tp, 2)
            return [(v[:rows].astype(f32) + got[:, a:b].astype(f32)).astype(bf16) for v, (a, b) in zip(total, spans)]

        first = add_up([down, down_a[1], down_a[2]])
        second = add_up([down_b[1], down_b[2], down_a[3]])
        third = add_up([down_b[3]])
        channel_out = [
            first[0],
            jnp.concatenate([first[1], second[0]], axis=1),
            jnp.concatenate([first[2], second[1]], axis=1),
            jnp.concatenate([second[2], third[0]], axis=1),
        ]
        r = rsqrt_mean(channel_out, width)
        result = [(middle[j].astype(f32) + channel_out[j].astype(f32) * r * gain[3][j]).astype(bf16) for j in range(n_fs)]
        return jnp.concatenate(slots(jnp.concatenate(result, axis=1)), axis=1)

    return local


def solution(mesh):
    n_grp, n_fs, n_tp = (mesh.shape[name] for name in ("grp", "fs", "tp"))
    small = (n_grp, n_fs, n_tp) == (2, 4, 4)
    return jax.shard_map(
        make_local(n_grp, n_fs, n_tp) if small else whole_axis,
        mesh=mesh,
        in_specs=(
            P(("grp", "fs", "tp"), None),
            P("fs", "tp"),
            P("tp"),
            P("tp", "fs"),
            P("fs", "tp"),
            P("tp", "fs"),
            P(),
        ),
        out_specs=P(("grp", "fs", "tp"), None),
        check_vma=False,
    )
```

```python
import jax
import jax.numpy as jnp
from jax import lax
from jax.sharding import PartitionSpec as P

PW = 1024
GROUPS = 4

norm_eps = 1e-06
pool_spans = (2, 4, 8, 16)


f32, bf16 = jnp.float32, jnp.bfloat16


def normalize(values, gain):
    upcast = values.astype(jnp.float32)
    return upcast * lax.rsqrt(jnp.mean(upcast * upcast, axis=-1, keepdims=True) + norm_eps) * gain


def pooling(mixed_in, first_channel):
    length = mixed_in.shape[0]
    upcast = mixed_in.astype(jnp.float32)
    running = jnp.cumsum(upcast, axis=0)
    position = jnp.arange(1, length + 1, dtype=jnp.float32)[:, None]
    channel = first_channel + jnp.arange(mixed_in.shape[1], dtype=jnp.int32)
    group_of = (channel // (PW // GROUPS))[None, :]
    average = jnp.zeros_like(upcast)
    for index, span in enumerate(pool_spans):
        lagged = jnp.pad(running, ((span, 0), (0, 0)))[:length]
        window_mean = (running - lagged) / jnp.minimum(position, float(span))
        average = jnp.where(group_of == index, window_mean, average)
    return average - upcast


def whole_axis(tokens, mix_weight_in, pool_scale, mix_weight_out, up_weight, down_weight, gains):
    normed = normalize(tokens, gains[0]).astype(jnp.bfloat16)
    gathered = lax.all_gather(normed, "tp", axis=0, tiled=True)
    mixed_acc = jnp.dot(
        gathered,
        lax.all_gather(mix_weight_in, "fs", axis=0, tiled=True),
        preferred_element_type=jnp.float32,
    )
    weight_out = lax.all_gather(mix_weight_out, "fs", axis=1, tiled=True)
    mixed_in = mixed_acc.astype(jnp.bfloat16)
    first_channel = lax.axis_index("tp") * mix_weight_in.shape[1]
    scaled = (pooling(mixed_in, first_channel) * pool_scale).astype(jnp.bfloat16)
    picked = scaled
    mixer_out = lax.psum_scatter(
        jnp.dot(picked, weight_out, preferred_element_type=jnp.float32).astype(jnp.bfloat16),
        "tp",
        scatter_dimension=0,
        tiled=True,
    )
    middle = (tokens.astype(jnp.float32) + normalize(mixer_out, gains[1])).astype(jnp.bfloat16)
    normed_two = normalize(middle, gains[2]).astype(jnp.bfloat16)
    gathered_two = lax.all_gather(normed_two, "tp", axis=0, tiled=True)
    whole_up = lax.all_gather(up_weight, "fs", axis=0, tiled=True)
    hidden_pre = jnp.dot(gathered_two, whole_up, preferred_element_type=jnp.float32)
    hidden_pre = jax.nn.relu(hidden_pre)
    squared = (hidden_pre * hidden_pre).astype(jnp.bfloat16)
    whole_down = lax.all_gather(down_weight, "fs", axis=1, tiled=True)
    picked = squared
    channel_out = lax.psum_scatter(
        jnp.dot(picked, whole_down, preferred_element_type=jnp.float32).astype(jnp.bfloat16),
        "tp",
        scatter_dimension=0,
        tiled=True,
    )
    return (middle.astype(jnp.float32) + normalize(channel_out, gains[3])).astype(jnp.bfloat16)


def rsqrt_mean(blocks, width):
    total = sum(jnp.sum(b.astype(f32) * b.astype(f32), axis=-1, keepdims=True) for b in blocks)
    return lax.rsqrt(total / width + norm_eps)


def tie(value, *after):
    return lax.optimization_barrier((value,) + after)[0] if after else value


def dot(a, b):
    return jnp.dot(a, b, preferred_element_type=f32)


def make_local(n_grp, n_fs, n_tp):
    def swap(value, axis, n, bit):
        return lax.ppermute(value, axis, [(i, i ^ bit) for i in range(n)])

    def local(tokens, mix_in, pool_scale, mix_out, up, down, gains):
        g, z, t = lax.axis_index("grp"), lax.axis_index("fs"), lax.axis_index("tp")
        rows, width = tokens.shape
        col = width // n_fs
        channels = mix_in.shape[1]
        part = channels // n_grp
        ff = up.shape[1] // n_grp

        def slots(value):
            blocks = [value[..., k * col:(k + 1) * col] for k in range(n_fs)]
            for bit in (2, 1):
                blocks = [jnp.where((z & bit) != 0, blocks[k ^ bit], blocks[k]) for k in range(n_fs)]
            return blocks

        def gather_fs(value):
            two = swap(value, "fs", n_fs, 2)
            one = swap(value, "fs", n_fs, 1)
            return [value, one, two]

        def last_hop(pieces, *after):
            pieces.append(swap(tie(pieces[2], *after), "fs", n_fs, 1))

        mi = gather_fs(lax.dynamic_slice_in_dim(mix_in, g * part, part, axis=1))
        mo = gather_fs(lax.dynamic_slice_in_dim(mix_out, g * part, part, axis=0))
        up = gather_fs(lax.dynamic_slice_in_dim(up, g * ff, ff, axis=1))
        for pieces in (mi, mo, up):
            last_hop(pieces)
        down = lax.dynamic_slice_in_dim(down, g * ff, ff, axis=0)
        down_a = gather_fs(down[:, :col // 2])
        down_b = gather_fs(down[:, col // 2:])

        w_in = jnp.concatenate(mi, axis=0)
        w_in = jnp.concatenate([w_in, swap(w_in, "grp", n_grp, 1)], axis=1)
        w_out = jnp.concatenate(mo, axis=1)
        w_out = jnp.concatenate([w_out, swap(w_out, "grp", n_grp, 1)], axis=0)

        gain = [slots(gains[k:k + 1]) for k in range(4)]
        x = slots(tokens)
        r = rsqrt_mean([tokens], width)
        normed = jnp.concatenate([(x[j].astype(f32) * r * gain[0][j]).astype(bf16) for j in range(n_fs)], axis=1)
        gathered = jnp.concatenate([normed, swap(normed, "tp", n_tp, 2)], axis=0)
        gathered = jnp.concatenate([gathered, swap(gathered, "tp", n_tp, 1)], axis=0)
        order = (0, 2, 1, 3)

        scale = [lax.dynamic_slice_in_dim(pool_scale, (g ^ k) * part, part) for k in range(n_grp)]
        scale = jnp.concatenate(scale)[None, :]
        index = jnp.arange(rows, dtype=jnp.int32)
        position = jnp.concatenate([(t ^ k) * rows + index for k in order])
        group = PW // GROUPS
        mine = (t * channels) // group
        span = jnp.int32(pool_spans[0])
        for k in range(1, GROUPS):
            span = jnp.where(mine == k, pool_spans[k], span)
        lag = position[:, None] - position[None, :]
        ones = ((lag >= 0) & (lag < span)).astype(bf16)
        count = jnp.minimum(position + 1, span).astype(f32)[:, None]

        mixed = dot(gathered, w_in).astype(bf16)
        average = dot(ones, mixed) / count
        scaled = ((average - mixed.astype(f32)) * scale).astype(bf16)
        half = 2 * rows
        sent = swap(dot(scaled[half:], w_out).astype(bf16), "tp", n_tp, 1)
        partial = (dot(scaled[:half], w_out) + sent.astype(f32)).astype(bf16)
        sent = swap(partial[rows:], "tp", n_tp, 2)
        partial = (partial[:rows].astype(f32) + sent.astype(f32)).astype(bf16)

        mixer_out = [partial[:, k * col:(k + 1) * col] for k in range(n_fs)]
        r = rsqrt_mean(mixer_out, width)
        middle = [(x[j].astype(f32) + mixer_out[j].astype(f32) * r * gain[1][j]).astype(bf16) for j in range(n_fs)]
        r = rsqrt_mean(middle, width)
        normed_two = [(middle[j].astype(f32) * r * gain[2][j]).astype(bf16) for j in range(n_fs)]

        left = jnp.concatenate(normed_two[:2], axis=1)
        right = jnp.concatenate(normed_two[2:], axis=1)
        left = jnp.concatenate([left, swap(left, "tp", n_tp, 2)], axis=0)
        left_far = swap(left, "grp", n_grp, 1)
        right_grp = swap(right, "grp", n_grp, 1)
        right_far = swap(jnp.concatenate([right, right_grp], axis=0), "tp", n_tp, 2)
        chips = jnp.concatenate(
            [
                jnp.concatenate([left, left_far], axis=0),
                jnp.concatenate([right, right_far[:rows], right_grp, right_far[rows:]], axis=0),
            ],
            axis=1,
        )
        everything = jnp.concatenate([chips, swap(chips, "tp", n_tp, 1)], axis=0)

        hidden = sum(dot(everything[:, j * col:(j + 1) * col], up[j]) for j in range(n_fs))
        hidden = jnp.maximum(hidden, 0.0)
        squared = (hidden * hidden).astype(bf16)

        def add_up(weights):
            half = 4 * rows
            sent = jnp.concatenate([dot(squared[half:], w).astype(bf16) for w in weights], axis=1)
            got = swap(sent, "tp", n_tp, 1)
            spans, at = [], 0
            for w in weights:
                spans.append((at, at + w.shape[1]))
                at += w.shape[1]
            total = [(dot(squared[:half], w) + got[:, a:b].astype(f32)).astype(bf16) for w, (a, b) in zip(weights, spans)]
            got = swap(jnp.concatenate([v[half // 2:] for v in total], axis=1), "grp", n_grp, 1)
            total = [(v[:half // 2].astype(f32) + got[:, a:b].astype(f32)).astype(bf16) for v, (a, b) in zip(total, spans)]
            stage.append(total[0])
            got = swap(jnp.concatenate([v[rows:] for v in total], axis=1), "tp", n_tp, 2)
            return [(v[:rows].astype(f32) + got[:, a:b].astype(f32)).astype(bf16) for v, (a, b) in zip(total, spans)]

        stage = []
        last_hop(down_a, squared)
        last_hop(down_b, squared)
        first = add_up([down, down_a[1], down_a[2]])
        second = add_up([tie(v, stage[0]) for v in down_b[1:3]])
        third = add_up([tie(down_a[3], stage[1])])
        fourth = add_up([tie(down_b[3], stage[2])])
        channel_out = [
            first[0],
            jnp.concatenate([first[1], second[0]], axis=1),
            jnp.concatenate([first[2], second[1]], axis=1),
            jnp.concatenate([third[0], fourth[0]], axis=1),
        ]
        r = rsqrt_mean(channel_out, width)
        result = [(middle[j].astype(f32) + channel_out[j].astype(f32) * r * gain[3][j]).astype(bf16) for j in range(n_fs)]
        return jnp.concatenate(slots(jnp.concatenate(result, axis=1)), axis=1)

    return local


def solution(mesh):
    n_grp, n_fs, n_tp = (mesh.shape[name] for name in ("grp", "fs", "tp"))
    small = (n_grp, n_fs, n_tp) == (2, 4, 4)
    return jax.shard_map(
        make_local(n_grp, n_fs, n_tp) if small else whole_axis,
        mesh=mesh,
        in_specs=(
            P(("grp", "fs", "tp"), None),
            P("fs", "tp"),
            P("tp"),
            P("tp", "fs"),
            P("fs", "tp"),
            P("tp", "fs"),
            P(),
        ),
        out_specs=P(("grp", "fs", "tp"), None),
        check_vma=False,
    )
```
